32 devices in a mesh: grp: 2 (over y), dp: 2 (over x), kv: 4 (over z), tp: 2 (over core).
Axes of the slice: x: 2, y: 2, z: 4, core: 2. Of those that a mesh axis runs over, the one named last changes fastest.
Arguments:
- resid: bfloat16 [12, 2048], P(('grp', 'dp'), ('kv', 'tp')), parts along dimension 0, may hold values from -7 to 7
- keys_cache: bfloat16 [12, 4096, 256], P(('grp', 'dp'), 'kv', 'tp'), parts along dimension 0, may hold values from -310 to 310
- values_cache: bfloat16 [12, 4096, 256], P(('grp', 'dp'), 'kv', 'tp'), parts along dimension 0, may hold values from -6 to 6
- gates_cache: float32 [12, 4096, 4], P(('grp', 'dp'), 'kv', 'tp'), parts along dimension 0, may hold values from -1044 to 0, as said below
- norm_gain: float32 [2048], replicated, may hold values from 0.1 to 1.9
- w_query: bfloat16 [2048, 2048], P('kv', 'tp'), may hold values from -0.125 to 0.125
- w_key: bfloat16 [2048, 256], P('kv', 'tp'), may hold values from -0.125 to 0.125
- w_value: bfloat16 [2048, 256], P('kv', 'tp'), may hold values from -0.5 to 0.5
- w_forget: bfloat16 [2048, 4], replicated, may hold values from -0.125 to 0.125
- forget_bias: float32 [4], replicated, may hold values from -3 to 1
- w_out: bfloat16 [2048, 2048], P('tp', 'kv'), may hold values from -0.5 to 0.5
- mlp_gain: float32 [2048], replicated, may hold values from 0.1 to 1.9
- w_up: bfloat16 [2048, 8192], P('kv', 'tp'), may hold values from -0.125 to 0.125
- w_down: bfloat16 [8192, 2048], P('tp', 'kv'), may hold values from -0.0625 to 0.0625
Outputs:
- next_resid: bfloat16 [12, 2048], P(('grp', 'dp'), ('kv', 'tp')), parts along dimension 0
The draws below stay inside these ranges and needn't reach their ends.
There are 2 independent parts, one for each index of `grp`. The reference program is written for one: setup_inputs(seed, part) draws one part's arguments, and reference() takes and returns one part's arrays. A program takes and returns all parts, laid end to end along the dimension named above; an argument that names none is the same for every part. Nothing has to cross between parts.
Inputs may be any that keep to these rules, and one draw needn't show every extreme that they name: gates_cache[b, p, g] is the sum of the log forget gates of the cached positions after p, so it never falls along the positions and is 0 at the last one.
All inputs are finite; a program needn't handle non-finite values.
Results may differ from the reference program's by a relative error of at most 0.028.
Values may be sent and summed in bfloat16 or wider, within the bound.
No kernel may reach another device: no remote copies, remote signals or barrier semaphores. Data moves between devices by JAX's collectives and lax.ppermute only.
A program may use at most 64 MiB of HBM per device.

```python
import jax
import jax.numpy as jnp
from jax import lax

D = 2048
HEADS = 32
LOOKUP_GROUPS = 4
HEAD = 64
FF = 8192
CTX_DEV = 1024
TOTAL_STRINGS = 6
STORED_SLOTS = 4096
QW = 2048
KW = 256
N_TP = 2


def draw_resid(key, part):
    key_base, key_cols, key_rows = jax.random.split(jax.random.fold_in(key, 5), 3)
    columns = jnp.arange(D, dtype=jnp.float32) / D
    col_scale = jnp.exp(jnp.log(0.1) + jnp.log(5.0) * columns + 0.3 * jax.random.uniform(key_cols, (D,), jnp.float32, -1.0, 1.0))
    base = jnp.clip(jax.random.normal(key_base, (TOTAL_STRINGS, D), jnp.float32), -5.0, 5.0)
    row_scale = jnp.exp(jax.random.uniform(key_rows, (TOTAL_STRINGS, 1), jnp.float32, 0.0, jnp.log(2.0)))
    return (base * col_scale * row_scale).astype(jnp.bfloat16)


def draw_keys_cache(key, part):
    key_base = jax.random.fold_in(jax.random.fold_in(key, 3), 0)
    keys = jnp.clip(jax.random.normal(key_base, (TOTAL_STRINGS, STORED_SLOTS, KW), jnp.float32), -5.0, 5.0)
    return keys.astype(jnp.bfloat16)


def draw_gates_cache(key, part):
    seed_gradual, seed_speed, seed_quick, seed_tile, seed_jitter, seed_spike, seed_discard = jax.random.split(jax.random.fold_in(key, 9), 7)
    pick = jax.random.uniform(seed_gradual, (TOTAL_STRINGS, 1, LOOKUP_GROUPS), jnp.float32)
    slow = pick < 0.5
    slow_rate = jax.random.uniform(seed_speed, (TOTAL_STRINGS, 1, LOOKUP_GROUPS), jnp.float32, 0.3, 1.0) / STORED_SLOTS
    fast_rate = 1.0 / jax.random.uniform(seed_quick, (TOTAL_STRINGS, 1, LOOKUP_GROUPS), jnp.float32, 25.0, 60.0)
    rate = jnp.where(slow, slow_rate, fast_rate)
    factor = jnp.exp(jax.random.uniform(seed_tile, (TOTAL_STRINGS, STORED_SLOTS // CTX_DEV, LOOKUP_GROUPS), jnp.float32, jnp.log(0.5), jnp.log(2.0)))
    factor = jnp.repeat(factor, CTX_DEV, axis=1)
    noise = jax.random.uniform(seed_jitter, (TOTAL_STRINGS, STORED_SLOTS, LOOKUP_GROUPS), jnp.float32, 0.5, 1.5)
    log_increments = -rate * factor * noise
    spike_magnitude = jax.random.uniform(seed_spike, (TOTAL_STRINGS, STORED_SLOTS, LOOKUP_GROUPS), jnp.float32) < 2.0 / STORED_SLOTS
    discard_proportion = jnp.log(jax.random.uniform(seed_discard, (TOTAL_STRINGS, STORED_SLOTS, LOOKUP_GROUPS), jnp.float32, 0.5, 0.8))
    log_increments = log_increments + jnp.where(spike_magnitude, discard_proportion, 0.0)
    after = jnp.flip(jnp.cumsum(jnp.flip(log_increments, 1), 1), 1) - log_increments
    return after


def shard_levels(own_key, dims, cuts, least, top_value):
    factor_of, own = 1.0, jax.random.fold_in(own_key, 6)
    for position, blocks in cuts:
        heights = jnp.exp(jax.random.uniform(jax.random.fold_in(own, position), (blocks,), jnp.float32, least / len(cuts), top_value / len(cuts)))
        factor_of = factor_of * jnp.repeat(heights, dims[position] // blocks).reshape([-1 if axis == position else 1 for axis in range(len(dims))])
    return factor_of


def scatter_about(own_key, extent, scale, bound, cuts=(), held_as=jnp.bfloat16):
    result = scale * jax.random.normal(own_key, extent, jnp.float32)
    if cuts:
        result = result * shard_levels(own_key, extent, cuts, -0.22, 0.18)
    return jnp.clip(result, -bound, bound).astype(held_as)


def setup_inputs(seed: int = 0, part: int = 0) -> dict:
    splits = jax.random.split(jax.random.key(seed), 15)
    part_splits = jax.random.split(jax.random.fold_in(splits[14], part), 15)
    resid = draw_resid(jax.random.fold_in(jax.random.fold_in(splits[14], part), 71), part)
    keys_cache = draw_keys_cache(jax.random.fold_in(jax.random.fold_in(splits[14], part), 71), part)
    values_cache = scatter_about(part_splits[2], (TOTAL_STRINGS, STORED_SLOTS, KW), 1.0, 6.0, ((0, 2), (1, 4), (2, 2)))
    gates_cache = draw_gates_cache(jax.random.fold_in(jax.random.fold_in(splits[14], part), 71), part)
    norm_gain = jnp.clip(1.0 + 0.18 * jax.random.normal(splits[4], (D,), jnp.float32), 0.1, 1.9)
    w_query = scatter_about(splits[5], (D, QW), D ** -0.5, 0.125, ((0, 4), (1, 2)))
    w_key = scatter_about(splits[6], (D, KW), D ** -0.5, 0.125, ((0, 4), (1, 2)))
    w_value = scatter_about(splits[7], (D, KW), (D // 16) ** -0.5, 0.5, ((0, 4), (1, 2)))
    w_forget = scatter_about(splits[8], (D, LOOKUP_GROUPS), D ** -0.5, 0.125)
    forget_bias = jnp.clip(jax.random.uniform(splits[9], (LOOKUP_GROUPS,), jnp.float32, -3.0, 1.0), -3.0, 1.0)
    w_out = scatter_about(splits[10], (QW, D), (QW // 16) ** -0.5, 0.5, ((0, 2), (1, 4)))
    mlp_gain = jnp.clip(1.0 + 0.18 * jax.random.normal(splits[11], (D,), jnp.float32), 0.1, 1.9)
    w_up = scatter_about(splits[12], (D, FF), D ** -0.5, 0.125, ((0, 4), (1, 2)))
    w_down = scatter_about(splits[13], (FF, D), FF ** -0.5, 0.0625, ((0, 2), (1, 4)))
    return {"resid": resid, "keys_cache": keys_cache, "values_cache": values_cache, "gates_cache": gates_cache, "norm_gain": norm_gain, "w_query": w_query, "w_key": w_key, "w_value": w_value, "w_forget": w_forget, "forget_bias": forget_bias, "w_out": w_out, "mlp_gain": mlp_gain, "w_up": w_up, "w_down": w_down}


EPS = 1e-06

def scaled_rows(source, gain_vector):
    values32 = source.astype(jnp.float32)
    inverse = lax.rsqrt(lax.optimization_barrier(jnp.mean(values32 * values32, axis=1, keepdims=True)) + EPS)
    scaled = (values32 * gain_vector).astype(jnp.bfloat16)
    return (scaled, inverse)

def attend_sequence(inputs):
    query, key_new, value_new, log_forget, cached_keys, cached_values, cached_gates = inputs
    group_size = HEADS // LOOKUP_GROUPS
    score_scale = HEAD ** (-0.5)
    query32 = query.astype(jnp.float32).reshape(LOOKUP_GROUPS, group_size, HEAD)
    keys32 = cached_keys.astype(jnp.float32).reshape(STORED_SLOTS, LOOKUP_GROUPS, HEAD)
    values32 = cached_values.astype(jnp.float32).reshape(STORED_SLOTS, LOOKUP_GROUPS, HEAD)
    scores = jnp.einsum('gjd,pgd->gjp', query32, keys32) * score_scale
    scores = scores + (jnp.transpose(cached_gates) + log_forget[:, None])[:, None, :]
    fresh = jnp.einsum('gjd,gd->gj', query32, key_new.astype(jnp.float32).reshape(LOOKUP_GROUPS, HEAD)) * score_scale
    new_peak = jnp.maximum(lax.optimization_barrier(jnp.max(scores, axis=2)), fresh)
    weights = jnp.exp(scores - new_peak[:, :, None])
    own_weight = jnp.exp(fresh - new_peak)
    totals = lax.optimization_barrier(jnp.sum(weights, axis=2)) + own_weight
    rounded = lax.optimization_barrier(weights.astype(jnp.bfloat16)).astype(jnp.float32)
    own_rounded = lax.optimization_barrier(own_weight.astype(jnp.bfloat16)).astype(jnp.float32)
    mixed = jnp.einsum('gjp,pgd->gjd', rounded, values32)
    mixed = mixed + own_rounded[:, :, None] * value_new.astype(jnp.float32).reshape(LOOKUP_GROUPS, 1, HEAD)
    return (mixed / totals[:, :, None]).astype(jnp.bfloat16).reshape(HEADS * HEAD)

def split_product(left, right, pieces):
    width_piece = left.shape[1] // pieces
    total = jnp.zeros((left.shape[0], right.shape[1]), jnp.float32)
    for shard_index in range(pieces):
        lower = shard_index * width_piece
        part = jnp.dot(left[:, lower:lower + width_piece], right[lower:lower + width_piece], preferred_element_type=jnp.float32)
        total = total + part.astype(jnp.bfloat16).astype(jnp.float32)
    return total

def reference(resid, keys_cache, values_cache, gates_cache, norm_gain, w_query, w_key, w_value, w_forget, forget_bias, w_out, mlp_gain, w_up, w_down):
    scaled, inverse = scaled_rows(resid, norm_gain)
    query = (jnp.dot(scaled, w_query, preferred_element_type=jnp.float32) * inverse).astype(jnp.bfloat16)
    key_new = (jnp.dot(scaled, w_key, preferred_element_type=jnp.float32) * inverse).astype(jnp.bfloat16)
    value_new = (jnp.dot(scaled, w_value, preferred_element_type=jnp.float32) * inverse).astype(jnp.bfloat16)
    log_forget = jax.nn.log_sigmoid(jnp.dot(scaled, w_forget, preferred_element_type=jnp.float32) * inverse + forget_bias)
    attended = lax.map(attend_sequence, (query, key_new, value_new, log_forget, keys_cache, values_cache, gates_cache))
    middle = (resid.astype(jnp.float32) + split_product(attended, w_out, N_TP)).astype(jnp.bfloat16)
    scaled_mid, inverse_mid = scaled_rows(middle, mlp_gain)
    up_total = jnp.dot(scaled_mid, w_up, preferred_element_type=jnp.float32) * inverse_mid
    hidden = jnp.square(jax.nn.relu(up_total)).astype(jnp.bfloat16)
    return (middle.astype(jnp.float32) + split_product(hidden, w_down, N_TP)).astype(jnp.bfloat16)
```

```python
import functools

import jax
import jax.numpy as jnp
from jax import lax
from jax.experimental import pallas as pl
from jax.experimental.pallas import tpu as pltpu
from jax.sharding import PartitionSpec as P

EPS = 1e-06
LANES = 128
GRANT = 12 * 1024 * 1024

F32 = jnp.float32
BF16 = jnp.bfloat16


def dot(left, right):
    return jnp.dot(left, right, preferred_element_type=F32)


def dot_t(left, right):
    return lax.dot_general(left, right, (((1,), (1,)), ((), ())), preferred_element_type=F32)


def tree_sum(parts):
    while len(parts) > 1:
        parts = [parts[k] + parts[k + 1] for k in range(0, len(parts), 2)]
    return parts[0]


def call(kernel, out, *operands, **static):
    return pl.pallas_call(
        functools.partial(kernel, **static),
        out_shape=out,
        compiler_params=pltpu.CompilerParams(vmem_limit_bytes=GRANT),
    )(*operands)


def swap(value, axis, step):
    size = lax.axis_size(axis)
    return lax.ppermute(value, axis, [(k, k ^ step) for k in range(size)])


def exchange(value, axis):
    return [value] + [swap(value, axis, step) for step in range(1, lax.axis_size(axis))]


def block_rows(own, other):
    first = lax.axis_index("tp") == 0
    own, other = own.astype(F32), other.astype(F32)
    return jnp.concatenate([jnp.where(first, own, other), jnp.where(first, other, own)], axis=1)


def project_kernel(own, other, gain, w_query, w_key, w_value, w_forget, out):
    width, qw = w_query.shape
    kw = w_key.shape[1]
    groups = w_forget.shape[0]
    offset = pl.multiple_of(lax.axis_index("kv") * width, LANES)
    rows = block_rows(own[...], other[...])
    scaled = (rows * gain[:, pl.ds(offset, width)]).astype(BF16)
    out[:, :qw] = dot(scaled, w_query[...])
    out[:, qw : qw + kw] = dot(scaled, w_key[...])
    out[:, qw + kw : qw + 2 * kw] = dot(scaled, w_value[...])
    tail = qw + 2 * kw
    out[:, tail:] = jnp.zeros((out.shape[0], LANES), F32)
    out[:, tail : tail + groups] = dot_t(scaled, w_forget[:, pl.ds(offset, width)])
    out[:, tail + groups : tail + groups + 1] = jnp.sum(rows * rows, axis=1, keepdims=True)


def attend_kernel(*refs, count, features):
    parts = refs[:count]
    keys, values, gates, bias, out = refs[count:]
    batch, _, kw = keys.shape
    local = gates.shape[1]
    groups = bias.shape[1]
    head = kw // local
    tail = parts[0].shape[1] - LANES
    qw = tail - 2 * kw
    pairs = qw // kw
    scale = head ** (-0.5)
    total = tree_sum([part[...] for part in parts])
    inverse = lax.rsqrt(total[:, tail + groups : tail + groups + 1] / features + EPS)
    query = (total[:, :qw] * inverse).astype(BF16).astype(F32)
    key_new = (total[:, qw : qw + kw] * inverse).astype(BF16).astype(F32)
    value_new = (total[:, qw + kw : tail] * inverse).astype(BF16).astype(F32)
    logit = total[:, tail : tail + groups] * inverse + bias[...]
    forget_all = jnp.minimum(logit, 0.0) - jnp.log(1.0 + jnp.exp(-jnp.abs(logit)))
    column = lax.broadcasted_iota(jnp.int32, forget_all.shape, 1) - lax.axis_index("tp") * local
    forget = [
        jnp.sum(jnp.where(column == g, forget_all, 0.0), axis=1, keepdims=True) for g in range(local)
    ]
    holds_new = lax.axis_index("kv") == 0
    low = lax.broadcasted_iota(jnp.int32, (pairs, kw), 1) < head
    first = lax.broadcasted_iota(jnp.int32, (pairs, kw), 0) < pairs // 2
    first_col = lax.broadcasted_iota(jnp.int32, (pairs, 1), 0) < pairs // 2
    lane = lax.broadcasted_iota(jnp.int32, (pairs, LANES), 1)
    stats = jnp.zeros((pairs, LANES), F32)
    for b in range(batch):
        straight = jnp.concatenate(
            [query[b : b + 1, k * kw : (k + 1) * kw] for k in range(pairs)], axis=0
        )
        rolled = pltpu.roll(straight, head, 1)
        even = jnp.where(first, jnp.where(low, straight, 0.0), jnp.where(low, 0.0, rolled))
        odd = jnp.where(first, jnp.where(low, rolled, 0.0), jnp.where(low, 0.0, straight))
        heads = jnp.concatenate([even, odd], axis=0)
        gate = jnp.where(first_col, gates[b, 0:1, :], gates[b, 1:2, :])
        scores = dot_t(heads.astype(BF16), keys[b]) * scale + jnp.concatenate([gate, gate], axis=0)
        decay = jnp.where(first_col, forget[0][b : b + 1], forget[1][b : b + 1])
        decay = jnp.concatenate([decay, decay], axis=0)
        fresh = jnp.sum(heads * key_new[b : b + 1], axis=1, keepdims=True) * scale
        fresh = jnp.where(holds_new, fresh, -jnp.inf)
        peak = jnp.maximum(jnp.max(scores, axis=1, keepdims=True) + decay, fresh)
        weights = jnp.exp(scores + (decay - peak))
        own = jnp.exp(fresh - peak)
        sums = jnp.sum(weights, axis=1, keepdims=True) + own
        mixed = dot(weights.astype(BF16), values[b])
        mixed = mixed + own.astype(BF16).astype(F32) * value_new[b : b + 1]
        even, odd = mixed[:pairs], mixed[pairs:]
        turned_even, turned_odd = pltpu.roll(even, head, 1), pltpu.roll(odd, head, 1)
        out[b * pairs : (b + 1) * pairs, :] = jnp.where(
            low, jnp.where(first, even, turned_even), jnp.where(first, turned_odd, odd)
        )
        for parity in range(2):
            cut = slice(parity * pairs, (parity + 1) * pairs)
            stats = jnp.where(lane == 2 * b + parity, peak[cut], stats)
            stats = jnp.where(lane == LANES // 2 + 2 * b + parity, sums[cut], stats)
    out[batch * pairs :, :] = stats


def output_kernel(*refs, count, batch):
    parts = [part[...] for part in refs[:count]]
    w_out, out = refs[count:]
    pairs = parts[0].shape[0] // (batch + 1)
    kw = parts[0].shape[1]
    stats = [part[batch * pairs :] for part in parts]
    peak = functools.reduce(jnp.maximum, stats)
    factors = [jnp.exp(stat - peak) for stat in stats]
    sums = tree_sum([pltpu.roll(s, LANES // 2, 1) * f for s, f in zip(stats, factors)])
    low = lax.broadcasted_iota(jnp.int32, (pairs, kw), 1) < kw // 2
    attended = []
    for b in range(batch):
        spread = lambda tile: jnp.where(
            low, tile[:, 2 * b : 2 * b + 1], tile[:, 2 * b + 1 : 2 * b + 2]
        )
        mixed = tree_sum(
            [p[b * pairs : (b + 1) * pairs] * spread(f) for p, f in zip(parts, factors)]
        )
        attended.append(mixed / spread(sums))
    rows = jnp.concatenate(
        [
            jnp.concatenate([tile[k : k + 1] for tile in attended], axis=0) for k in range(pairs)
        ],
        axis=1,
    ).astype(BF16)
    out[...] = dot(rows, w_out[...]).astype(BF16)


def up_kernel(own, other, part, part_other, gain, w_up, out, middle_out):
    width, ff = w_up.shape
    half = own.shape[1]
    offset = pl.multiple_of(lax.axis_index("kv") * width, LANES)
    branch = part[...].astype(F32) + part_other[...].astype(F32)
    middle = (block_rows(own[...], other[...]) + branch).astype(BF16).astype(F32)
    scaled = (middle * gain[:, pl.ds(offset, width)]).astype(BF16)
    out[:, :ff] = dot(scaled, w_up[...]).astype(BF16)
    squares = jnp.sum(middle * middle, axis=1, keepdims=True)
    coarse = squares.astype(BF16).astype(F32)
    lane = lax.broadcasted_iota(jnp.int32, (out.shape[0], LANES), 1)
    pair = jnp.where(lane == 0, coarse, jnp.where(lane == 1, squares - coarse, 0.0))
    out[:, ff:] = pair.astype(BF16)
    first = lax.axis_index("tp") == 0
    middle_out[...] = jnp.where(first, middle[:, :half], middle[:, half:])


def down_kernel(*refs, count, features):
    parts = refs[:count]
    w_down, sent, kept = refs[count:]
    ff = w_down.shape[0]
    half = sent.shape[1]
    total = tree_sum([part[...].astype(F32) for part in parts])
    squares = total[:, ff : ff + 1] + total[:, ff + 1 : ff + 2]
    inverse = lax.rsqrt(squares / features + EPS)
    hidden = jnp.square(jnp.maximum(total[:, :ff] * inverse, 0.0)).astype(BF16)
    down = dot(hidden, w_down[...])
    first = lax.axis_index("tp") == 0
    sent[...] = jnp.where(first, down[:, half:], down[:, :half]).astype(BF16)
    kept[...] = jnp.where(first, down[:, :half], down[:, half:]).astype(BF16)


def shards(
    resid,
    keys_cache,
    values_cache,
    gates_cache,
    norm_gain,
    w_query,
    w_key,
    w_value,
    w_forget,
    forget_bias,
    w_out,
    mlp_gain,
    w_up,
    w_down,
):
    batch, half = resid.shape
    count = lax.axis_size("kv")
    features = norm_gain.shape[0]
    qw, kw, ff = w_query.shape[1], w_key.shape[1], w_up.shape[1]
    other = swap(resid, "tp", 1)
    packed = call(
        project_kernel,
        jax.ShapeDtypeStruct((batch, qw + 2 * kw + LANES), F32),
        resid,
        other,
        norm_gain[None, :],
        w_query,
        w_key,
        w_value,
        w_forget.T,
    )
    packed = call(
        attend_kernel,
        jax.ShapeDtypeStruct(((batch + 1) * (qw // kw), kw), F32),
        *exchange(packed, "kv"),
        keys_cache,
        values_cache,
        jnp.transpose(gates_cache, (0, 2, 1)),
        forget_bias[None, :],
        count=count,
        features=features,
    )
    part = call(
        output_kernel,
        jax.ShapeDtypeStruct((batch, w_out.shape[1]), BF16),
        *exchange(packed, "kv"),
        w_out,
        count=count,
        batch=batch,
    )
    packed, middle = call(
        up_kernel,
        (
            jax.ShapeDtypeStruct((batch, ff + LANES), BF16),
            jax.ShapeDtypeStruct((batch, half), F32),
        ),
        resid,
        other,
        part,
        swap(part, "tp", 1),
        mlp_gain[None, :],
        w_up,
    )
    sent, kept = call(
        down_kernel,
        (jax.ShapeDtypeStruct((batch, half), BF16), jax.ShapeDtypeStruct((batch, half), BF16)),
        *exchange(packed, "kv"),
        w_down,
        count=count,
        features=features,
    )
    mixer = kept.astype(F32) + swap(sent, "tp", 1).astype(F32)
    return (middle + mixer).astype(BF16)


def solution(mesh):
    in_specs = (
        P(("grp", "dp"), ("kv", "tp")),
        P(("grp", "dp"), "kv", "tp"),
        P(("grp", "dp"), "kv", "tp"),
        P(("grp", "dp"), "kv", "tp"),
        P(),
        P("kv", "tp"),
        P("kv", "tp"),
        P("kv", "tp"),
        P(),
        P(),
        P("tp", "kv"),
        P(),
        P("kv", "tp"),
        P("tp", "kv"),
    )
    out_specs = P(("grp", "dp"), ("kv", "tp"))
    return jax.shard_map(shards, mesh=mesh, in_specs=in_specs, out_specs=out_specs, check_vma=False)
```
